32 devices in a mesh: sp: 16 (over z, y, core), tp: 2 (over x).
Axes of the slice: x: 2, y: 2, z: 4, core: 2. Of those that a mesh axis runs over, the one named last changes fastest.
Arguments:
- tokens: bfloat16 [2048, 2048], P(('sp', 'tp')), may hold values from -16 to 16
- w_query: bfloat16 [2048, 1024], P(None, 'tp'), may hold values from -0.110485435 to 0.110485435
- w_key: bfloat16 [2048, 256], P(None, 'tp'), may hold values from -0.15467961 to 0.15467961
- w_value: bfloat16 [2048, 256], P(None, 'tp'), may hold values from -0.125 to 0.125
- cum_gate: float32 [2048, 16], P('sp', 'tp'), may hold values from -371 to 0, as said below
- w_out: bfloat16 [1024, 2048], replicated, may hold values from -0.1875 to 0.1875
Outputs:
- mixed: bfloat16 [2048, 2048], P(('sp', 'tp'))
The draws below stay inside these ranges and needn't reach their ends.
Inputs may be any that keep to these rules, and one draw needn't show every extreme that they name: `cum_gate`: each head's column does not rise along the positions.
All inputs are finite; a program needn't handle non-finite values.
Results may differ from the reference program's by a relative error of at most 0.012.
Values may be sent and summed in bfloat16 or wider, within the bound.
A program may use at most 64 MiB of HBM per device.

```python
import math
import jax
import jax.numpy as jnp
from jax import lax

D = 2048
QUERY_HEAD_COUNT = 16
KV_HEADS = 4
HEAD_DIM = 64
TOK_DEV = 128
SEQUENCE_TOKENS = 2048


cluster_count = 3


def query_matrix(key):
    base = jax.random.normal(jax.random.fold_in(key, 11), (D, QUERY_HEAD_COUNT * HEAD_DIM), jnp.float32)
    return jnp.clip(base, -5.0, 5.0) * D ** (-0.5)


def jump_places(key):
    source = jax.random.fold_in(key, 41)
    first = jax.random.randint(jax.random.fold_in(source, 1), (cluster_count,), TOK_DEV, SEQUENCE_TOKENS - 40)
    second = first + 2 + jax.random.randint(jax.random.fold_in(source, 2), (cluster_count,), 0, 30)
    return jnp.concatenate([first, second]).astype(jnp.int32)


def draw_w_query(key, part):
    return query_matrix(key).astype(jnp.bfloat16)


def draw_w_key(key, part):
    fresh = jax.random.normal(jax.random.fold_in(key, 12), (D, KV_HEADS * HEAD_DIM), jnp.float32)
    fresh = jnp.clip(fresh, -5.0, 5.0) * D ** (-0.5)
    return fresh.astype(jnp.bfloat16)


def draw_tokens(key, part):
    blocks = SEQUENCE_TOKENS // TOK_DEV
    offsets = jax.random.normal(jax.random.fold_in(key, 21), (blocks, D), jnp.float32)
    spread = jnp.repeat(jnp.clip(offsets, -3.0, 3.0) * 0.8, TOK_DEV, axis=0)
    base = jnp.clip(jax.random.normal(jax.random.fold_in(key, 22), (SEQUENCE_TOKENS, D), jnp.float32), -5.0, 5.0)
    return (base + spread).astype(jnp.bfloat16)


def draw_cum_gate(key, part):
    order = jax.random.permutation(jax.random.fold_in(key, 31), QUERY_HEAD_COUNT)
    fast = order < QUERY_HEAD_COUNT // 2
    fast_rate = jax.random.uniform(jax.random.fold_in(key, 32), (QUERY_HEAD_COUNT,), jnp.float32, 1.0 / 80.0, 1.0 / 30.0)
    gentle_decay_rate = jax.random.uniform(jax.random.fold_in(key, 33), (QUERY_HEAD_COUNT,), jnp.float32, 0.2, 0.6) / SEQUENCE_TOKENS
    rate = jnp.where(fast, fast_rate, gentle_decay_rate)
    blocks = SEQUENCE_TOKENS // TOK_DEV
    factor = jnp.exp(jax.random.uniform(jax.random.fold_in(key, 34), (blocks, 1), jnp.float32, math.log(0.4), math.log(2.5)))
    factor = jnp.repeat(factor, TOK_DEV, axis=0)
    rough = jax.random.uniform(jax.random.fold_in(key, 35), (SEQUENCE_TOKENS, QUERY_HEAD_COUNT), jnp.float32, 0.2, 1.8)
    gate_steps_added = -rate[None, :] * factor * rough
    places = jump_places(key)
    count = places.shape[0]
    taken = jax.random.randint(jax.random.fold_in(key, 36), (count, QUERY_HEAD_COUNT), 0, 4) < 3
    sizes = jnp.log(jax.random.uniform(jax.random.fold_in(key, 37), (count, QUERY_HEAD_COUNT), jnp.float32, 0.6, 0.8))
    jump_values = jnp.where(taken, sizes, 0.0)
    where_pos = jnp.arange(SEQUENCE_TOKENS, dtype=jnp.int32)[:, None]
    hits = where_pos == places[None, :]
    jump_added = jnp.sum(jnp.where(hits[:, :, None], jump_values[None, :, :], 0.0), axis=1)
    gate_steps_added = gate_steps_added + jump_added
    return jnp.cumsum(gate_steps_added, axis=0)


def block_scale(own_key, extent, shards, smallest, largest):
    level = 1.0
    for axis_at, shards_of in shards:
        heights = jax.random.uniform(jax.random.fold_in(jax.random.fold_in(own_key, 6), axis_at), (shards_of,), jnp.float32, smallest / len(shards), largest / len(shards))
        level = level * jnp.repeat(jnp.exp(heights), extent[axis_at] // shards_of).reshape((-1,) + (1,) * (len(extent) - 1 - axis_at))
    return level


def normal_values(own_key, dims, scale, reach, cuts=(), kind=jnp.bfloat16):
    level = block_scale(own_key, dims, cuts, -0.22, 0.18) if cuts else 1.0
    entries = jax.random.normal(own_key, dims, jnp.float32) * scale * level
    return jnp.minimum(jnp.maximum(entries, -reach), reach).astype(kind)


def setup_inputs(seed: int = 0) -> dict:
    splits = jax.random.split(jax.random.key(seed), 7)
    tokens = draw_tokens(jax.random.fold_in(splits[6], 71), 0)
    w_query = draw_w_query(jax.random.fold_in(splits[6], 71), 0)
    w_key = draw_w_key(jax.random.fold_in(splits[6], 71), 0)
    w_value = normal_values(splits[3], (D, KV_HEADS * HEAD_DIM), D ** -0.5, 0.125, ((1, 2),))
    cum_gate = draw_cum_gate(jax.random.fold_in(splits[6], 71), 0)
    w_out = normal_values(splits[5], (QUERY_HEAD_COUNT * HEAD_DIM, D), (QUERY_HEAD_COUNT * HEAD_DIM) ** -0.5, 0.1875)
    return dict(tokens=tokens, w_query=w_query, w_key=w_key, w_value=w_value, cum_gate=cum_gate, w_out=w_out)


NEG_FILL = -1e30


def reference(tokens, w_query, w_key, w_value, cum_gate, w_out):
    group = QUERY_HEAD_COUNT // KV_HEADS
    queries = jnp.dot(tokens, w_query, preferred_element_type=jnp.float32).astype(jnp.bfloat16)
    keys = jnp.dot(tokens, w_key, preferred_element_type=jnp.float32).astype(jnp.bfloat16)
    values = jnp.dot(tokens, w_value, preferred_element_type=jnp.float32).astype(jnp.bfloat16)
    query_four = queries.astype(jnp.float32).reshape(SEQUENCE_TOKENS, KV_HEADS, group, HEAD_DIM)
    key_three = keys.astype(jnp.float32).reshape(SEQUENCE_TOKENS, KV_HEADS, HEAD_DIM)
    value_three = values.astype(jnp.float32).reshape(SEQUENCE_TOKENS, KV_HEADS, HEAD_DIM)
    gate_grouped = cum_gate.reshape(SEQUENCE_TOKENS, KV_HEADS, group)
    gate_keys = gate_grouped.transpose(1, 2, 0)
    positions = jnp.arange(SEQUENCE_TOKENS, dtype=jnp.int32)
    scale = HEAD_DIM ** -0.5

    def one_block(index):
        start = (index * TOK_DEV).astype(jnp.int32)
        query_tile_rows = lax.dynamic_slice_in_dim(query_four, start, TOK_DEV, 0)
        gate_block = lax.dynamic_slice_in_dim(gate_grouped, start, TOK_DEV, 0)
        scores = jnp.einsum("tkgd,rkd->tkgr", query_tile_rows, key_three) * scale
        scores = scores + gate_block[..., None] - gate_keys[None]
        query_pos = start + jnp.arange(TOK_DEV, dtype=jnp.int32)
        allowed = (positions[None, :] <= query_pos[:, None])[:, None, None, :]
        scores = jnp.where(allowed, scores, NEG_FILL)
        peak = jnp.max(scores, axis=-1, keepdims=True)
        raw = jnp.where(allowed, jnp.exp(scores - peak), 0.0)
        total = jnp.sum(raw, axis=-1)
        rounded = lax.optimization_barrier(raw.astype(jnp.bfloat16)).astype(jnp.float32)
        summed = jnp.einsum("tkgr,rkd->tkgd", rounded, value_three)
        return (summed / total[..., None]).astype(jnp.bfloat16).reshape(TOK_DEV, QUERY_HEAD_COUNT * HEAD_DIM)

    attended = lax.map(one_block, jnp.arange(SEQUENCE_TOKENS // TOK_DEV, dtype=jnp.int32))
    attended = attended.reshape(SEQUENCE_TOKENS, QUERY_HEAD_COUNT * HEAD_DIM)
    return jnp.dot(attended, w_out, preferred_element_type=jnp.float32).astype(jnp.bfloat16)
```

```python
import functools

import jax
import jax.numpy as jnp
from jax import lax
from jax.experimental import pallas as pl
from jax.experimental.pallas import tpu as pltpu
from jax.sharding import PartitionSpec as P

HEAD_DIM = 64
NEG_FILL = -1e30
LANES = 128
GATE_LANES = 32
BF = jnp.bfloat16
F32 = jnp.float32


def split3(x):
    hi = x.astype(BF).astype(F32)
    rest = x - hi
    mid = rest.astype(BF).astype(F32)
    low = (rest - mid).astype(BF).astype(F32)
    return hi, mid, low


def dims(n):
    chips = n // 2
    wide = max(b for b in range(1, chips + 1) if chips % b == 0 and b * b <= chips)
    return chips // wide, wide


def kernel(
    n,
    parts,
    tok_hbm,
    wq_hbm,
    wk_hbm,
    wv_hbm,
    gate_hbm,
    wo_hbm,
    out_ref,
    tok,
    wq,
    wk,
    wv,
    wo,
    gate,
    qrows,
    kv,
    gates,
    qg,
    run_max,
    run_sum,
    acc,
    att,
    att_in,
    load_sem,
    tok_send,
    tok_recv,
    att_send,
    att_recv,
    z_send,
    y_send,
    c_send,
    recv,
):
    deep, wide = dims(n)
    me = lax.axis_index("sp")
    tp = lax.axis_index("tp")
    core = lax.rem(me, 2)
    y = lax.rem(me // 2, wide)
    z = me // (2 * wide)
    rows = tok_hbm.shape[0]
    block = rows * parts
    heads = gate_hbm.shape[1]
    pc = wk_hbm.shape[1]
    local_kv = pc // HEAD_DIM
    group = heads // local_kv
    qc = heads * HEAD_DIM
    kw = pc if pc % LANES == 0 else 2 * pc
    cols = heads * block

    def index(zz, yy, cc):
        return (zz * wide + yy) * 2 + cc

    def peer(j):
        return lax.rem(tp + j, parts)

    loads = [
        pltpu.make_async_copy(src, dst, load_sem.at[i])
        for i, (src, dst) in enumerate(
            (
                (tok_hbm, tok.at[0]),
                (gate_hbm, gate),
                (wk_hbm, wk),
                (wv_hbm, wv),
                (wq_hbm, wq),
                (wo_hbm, wo),
            )
        )
    ]
    for load in loads:
        load.start()

    barrier = pltpu.get_barrier_semaphore()
    for j in range(1, parts):
        pl.semaphore_signal(barrier, inc=1, device_id={"tp": peer(j)})
    for j in range(1, deep):
        pl.semaphore_signal(barrier, inc=1, device_id={"sp": index(lax.rem(z + j, deep), y, core)})
    for j in range(1, wide):
        pl.semaphore_signal(barrier, inc=1, device_id={"sp": index(z, lax.rem(y + j, wide), core)})
    pl.semaphore_signal(barrier, inc=1, device_id={"sp": index(z, y, 1 - core)})
    loads[0].wait()
    loads[1].wait()

    turned = jnp.concatenate(
        [gate[pl.ds(pl.multiple_of(peer(j) * rows, rows), rows), :] for j in range(parts)], axis=0
    )
    hi, mid, low = split3(turned)
    fill = GATE_LANES - 3 * heads
    per_token = jnp.concatenate((hi, mid, low, jnp.ones((block, fill), F32)), axis=1)
    pack = LANES // GATE_LANES
    span = block // pack
    gates[me] = jnp.concatenate(
        [per_token[j * span : (j + 1) * span, :] for j in range(pack)], axis=1
    ).astype(BF)

    pl.semaphore_wait(barrier, parts - 1 + deep - 1 + wide - 1 + 1)

    tok_copies = []
    for j in range(1, parts):
        copy = pltpu.make_async_remote_copy(
            src_ref=tok.at[0],
            dst_ref=tok.at[parts - j],
            send_sem=tok_send.at[j],
            recv_sem=tok_recv.at[parts - j],
            device_id={"tp": peer(j)},
        )
        copy.start()
        tok_copies.append(copy)

    def view(item, who):
        if item == 0:
            return gates.at[who]
        if item == 1:
            return kv.at[who, pl.ds(0, rows)]
        return kv.at[who, pl.ds(rows, block - rows)]

    def push(item, who, send_sem, target):
        return pltpu.make_async_remote_copy(
            src_ref=view(item, who),
            dst_ref=view(item, who),
            send_sem=send_sem,
            recv_sem=recv.at[item, who],
            device_id={"sp": target},
        )

    def arrived(item, who):
        push(item, who, z_send.at[item, 0], me).wait_recv()

    def z_push(item, zz):
        return push(item, me, z_send.at[item, zz], index(zz, y, core))

    def y_push(item, zz, yy):
        return push(item, index(zz, y, core), y_send.at[item, zz, yy], index(z, yy, core))

    def c_push(item, zz, yy):
        return push(item, index(zz, yy, core), c_send.at[item, zz, yy], index(z, y, 1 - core))

    def loop(lo, hi, body):
        def step(i, carry):
            body(i)
            return carry

        lax.fori_loop(lo, hi, step, 0)

    def stage_own(item):
        loop(z + 1, deep, lambda zz: z_push(item, zz).start())
        loop(y + 1, wide, lambda yy: y_push(item, z, yy).start())

        @pl.when(core == 0)
        def _():
            c_push(item, z, y).start()

    def other_y(fn):
        loop(0, y, fn)
        loop(y + 1, wide, fn)

    def stage_z(item):
        def one(zz):
            arrived(item, index(zz, y, core))
            other_y(lambda yy: y_push(item, zz, yy).start())
            c_push(item, zz, y).start()

        loop(0, z, one)

    def stage_y(item):
        def at(zz, yy):
            arrived(item, index(zz, yy, core))
            c_push(item, zz, yy).start()

        loop(0, z, lambda zz: other_y(lambda yy: at(zz, yy)))
        loop(0, y, lambda yy: at(z, yy))

    def stage_c(item):
        def at(zz, yy):
            arrived(item, index(zz, yy, 1 - core))

        loop(0, z, lambda zz: loop(0, wide, lambda yy: at(zz, yy)))
        loop(0, y, lambda yy: at(z, yy))

        @pl.when(core == 1)
        def _():
            at(z, y)

    def drain(item):
        loop(z + 1, deep, lambda zz: z_push(item, zz).wait_send())
        loop(y + 1, wide, lambda yy: y_push(item, z, yy).wait_send())

        @pl.when(core == 0)
        def _():
            c_push(item, z, y).wait_send()

        def one(zz):
            other_y(lambda yy: y_push(item, zz, yy).wait_send())
            loop(0, wide, lambda yy: c_push(item, zz, yy).wait_send())

        loop(0, z, one)
        loop(0, y, lambda yy: c_push(item, z, yy).wait_send())

    stage_own(0)

    def project(j, with_kv):
        x = tok[j]
        if with_kv:
            key = jnp.dot(x, wk[...], preferred_element_type=F32)
            value = jnp.dot(x, wv[...], preferred_element_type=F32)
            kv[me, j * rows : (j + 1) * rows, :] = jnp.concatenate((key, value), axis=1).astype(BF)
        else:
            qrows[j * rows : (j + 1) * rows, :] = jnp.dot(
                x, wq[...], preferred_element_type=F32
            ).astype(BF)

    loads[2].wait()
    loads[3].wait()
    project(0, True)
    stage_own(1)
    loads[4].wait()
    project(0, False)
    stage_z(0)
    stage_z(1)
    stage_y(0)
    stage_y(1)
    for j in range(1, parts):
        tok_copies[parts - j - 1].wait_recv()
        project(j, True)
    stage_own(2)
    for j in range(1, parts):
        project(j, False)

    scale = HEAD_DIM ** (-0.5)
    lane = lax.broadcasted_iota(jnp.int32, (block, LANES), 1)
    query = qrows[...].astype(F32) * scale
    for h in range(heads):
        g = h // group
        place = []
        if g > 0:
            place.append(jnp.zeros((block, g * HEAD_DIM), F32))
        place.append(query[:, h * HEAD_DIM : (h + 1) * HEAD_DIM])
        if kw - (g + 1) * HEAD_DIM > 0:
            place.append(jnp.zeros((block, kw - (g + 1) * HEAD_DIM), F32))
        at_gate = (lane == h) | (lane == heads + h) | (lane == 2 * heads + h)
        side = jnp.where(at_gate, -1.0, 0.0)
        for i, piece in enumerate((hi, mid, low)):
            side = jnp.where(lane == 3 * heads + i, piece[:, h : h + 1], side)
        both = jnp.concatenate(place + [side], axis=1)
        qg[:, h * block : (h + 1) * block] = both.T.astype(BF)

    stage_c(0)
    stage_c(1)

    def unpack_gates(who):
        packed = gates[who].astype(F32)
        out = [packed] + [
            pltpu.roll(packed, LANES - j * GATE_LANES, 1) for j in range(1, pack)
        ]
        return jnp.concatenate(out, axis=0).astype(BF)

    def attend(first, count, lo, size, diagonal):
        width = count * size
        for_keys, for_gates = [], []
        for i in range(count):
            for_keys.append(kv[first + i, lo : lo + size, :])
            for_gates.append(unpack_gates(first + i)[lo : lo + size, :])
        keyval = jnp.concatenate(for_keys, axis=0) if count > 1 else for_keys[0]
        gate_part = jnp.concatenate(for_gates, axis=0) if count > 1 else for_gates[0]
        left = jnp.concatenate((keyval[:, :kw], gate_part), axis=1)
        value_t = keyval[:, pc:].astype(F32).T.astype(BF)
        for g in range(local_kv):
            at = slice(g * group * block, (g + 1) * group * block)
            scores = jnp.dot(left, qg[:, at], preferred_element_type=F32)
            if diagonal:
                turn = tp * rows
                key_pos = lax.rem(
                    lax.broadcasted_iota(jnp.int32, (width, block), 0) + turn, block
                )
                query_pos = lax.rem(
                    lax.broadcasted_iota(jnp.int32, (width, block), 1) + turn, block
                )
                allowed = jnp.concatenate([jnp.where(key_pos <= query_pos, 1.0, 0.0)] * group, axis=1) > 0.5
                scores = jnp.where(allowed, scores, NEG_FILL)
                new_max = jnp.max(scores, axis=0, keepdims=True)
            else:
                old_max = run_max[:, at]
                new_max = jnp.maximum(old_max, jnp.max(scores, axis=0, keepdims=True))
            weights = jnp.exp(scores - new_max)
            if diagonal:
                weights = jnp.where(allowed, weights, 0.0)
            total = jnp.sum(weights, axis=0, keepdims=True)
            gained = jnp.dot(
                value_t[g * HEAD_DIM : (g + 1) * HEAD_DIM, :],
                weights.astype(BF),
                preferred_element_type=F32,
            )
            if diagonal:
                run_sum[:, at] = total
                acc[:, at] = gained
            else:
                factor = jnp.exp(old_max - new_max)
                run_sum[:, at] = run_sum[:, at] * factor + total
                acc[:, at] = acc[:, at] * factor + gained
            run_max[:, at] = new_max

    def bits(limit):
        out = []
        size = 1
        while size < limit and size < 8:
            out.append(size)
            size *= 2
        return out[::-1]

    big = 8

    def big_part(lo, size):
        loop(0, me // big, lambda i: attend(i * big, big, lo, size, False))

    def small_part(lo, size):
        for count in bits(n):
            @pl.when(lax.rem(me // count, 2) == 1)
            def _():
                attend(me // (2 * count) * (2 * count), count, lo, size, False)

    attend(me, 1, 0, block, True)
    big_part(0, rows)
    stage_z(2)
    small_part(0, rows)
    stage_y(2)
    stage_c(2)
    big_part(rows, block - rows)
    small_part(rows, block - rows)

    done = acc[...] / run_sum[...]
    stacked = jnp.concatenate([done[:, h * block : (h + 1) * block] for h in range(heads)], axis=0)
    att[...] = stacked.T.astype(BF).reshape(parts, rows, qc)
    att_copies = []
    for j in range(1, parts):
        copy = pltpu.make_async_remote_copy(
            src_ref=att.at[j],
            dst_ref=att_in.at[parts - j],
            send_sem=att_send.at[j],
            recv_sem=att_recv.at[parts - j],
            device_id={"tp": peer(j)},
        )
        copy.start()
        att_copies.append(copy)
    loads[5].wait()

    def w_rows(j):
        return wo[pl.ds(pl.multiple_of(peer(j) * qc, qc), qc), :]

    mixed = jnp.dot(att[0], w_rows(0), preferred_element_type=F32)
    for j in range(1, parts):
        att_copies[parts - j - 1].wait_recv()
        mixed = mixed + jnp.dot(att_in[j], w_rows(j), preferred_element_type=F32)
    out_ref[...] = mixed.astype(BF)

    for copy in tok_copies + att_copies:
        copy.wait_send()
    for item in range(3):
        drain(item)


def shards(n, parts, tokens, w_query, w_key, w_value, cum_gate, w_out):
    deep, wide = dims(n)
    rows, width = tokens.shape
    block = rows * parts
    heads = cum_gate.shape[1]
    pc = w_key.shape[1]
    qc = w_query.shape[1]
    kw = pc if pc % LANES == 0 else 2 * pc
    cols = heads * block
    span = block * GATE_LANES // LANES
    dma = pltpu.SemaphoreType.DMA
    return pl.pallas_call(
        functools.partial(kernel, n, parts),
        out_shape=jax.ShapeDtypeStruct((rows, w_out.shape[1]), BF),
        in_specs=[pl.BlockSpec(memory_space=pl.ANY)] * 6,
        out_specs=pl.BlockSpec(memory_space=pltpu.VMEM),
        scratch_shapes=[
            pltpu.VMEM((parts, rows, width), BF),
            pltpu.VMEM(w_query.shape, BF),
            pltpu.VMEM(w_key.shape, BF),
            pltpu.VMEM(w_value.shape, BF),
            pltpu.VMEM(w_out.shape, BF),
            pltpu.VMEM(cum_gate.shape, F32),
            pltpu.VMEM((block, qc), BF),
            pltpu.VMEM((n, block, 2 * pc), BF),
            pltpu.VMEM((n, span, LANES), BF),
            pltpu.VMEM((kw + LANES, cols), BF),
            pltpu.VMEM((1, cols), F32),
            pltpu.VMEM((1, cols), F32),
            pltpu.VMEM((HEAD_DIM, cols), F32),
            pltpu.VMEM((parts, rows, qc), BF),
            pltpu.VMEM((parts, rows, qc), BF),
            dma((6,)),
            dma((parts,)),
            dma((parts,)),
            dma((parts,)),
            dma((parts,)),
            dma((3, deep)),
            dma((3, deep, wide)),
            dma((3, deep, wide)),
            dma((3, n)),
        ],
        compiler_params=pltpu.CompilerParams(
            collective_id=0, has_side_effects=True, vmem_limit_bytes=48 * 1024 * 1024
        ),
    )(tokens, w_query, w_key, w_value, cum_gate, w_out)


def solution(mesh):
    n, parts = mesh.shape["sp"], mesh.shape["tp"]
    placed = (
        P(("sp", "tp"), None),
        P(None, "tp"),
        P(None, "tp"),
        P(None, "tp"),
        P("sp", "tp"),
        P(),
    )
    return jax.shard_map(
        functools.partial(shards, n, parts),
        mesh=mesh,
        in_specs=placed,
        out_specs=P(("sp", "tp"), None),
        check_vma=False,
    )
```

```python
import functools
import math

import jax
import jax.numpy as jnp
from jax import lax
from jax.experimental import pallas as pl
from jax.experimental.pallas import tpu as pltpu
from jax.sharding import PartitionSpec as P

HEAD_DIM = 64
NEG_FILL = -1e30
LANES = 128
GATE_LANES = 32
VMEM_LIMIT = 67_043_328
BF = jnp.bfloat16
F32 = jnp.float32


def split3(x):
    hi = x.astype(BF).astype(F32)
    rest = x - hi
    mid = rest.astype(BF).astype(F32)
    low = (rest - mid).astype(BF).astype(F32)
    return hi, mid, low


def dims(n):
    chips = n // 2
    wide = max(b for b in range(1, chips + 1) if chips % b == 0 and b * b <= chips)
    return chips // wide, wide


def chunk_count(parts):
    return 1


def kernel(
    n,
    parts,
    tok_hbm,
    wq_hbm,
    wk_hbm,
    wv_hbm,
    gate_hbm,
    wo_hbm,
    out_ref,
    tok,
    wq,
    wkv,
    wo,
    gate_t,
    gate,
    qrows,
    kv,
    gates,
    sides,
    qg,
    run_max,
    run_sum,
    acc,
    att,
    att_in,
    load_sem,
    tok_send,
    tok_recv,
    att_send,
    att_recv,
    z_send,
    y_send,
    c_send,
    recv,
):
    deep, wide = dims(n)
    me = lax.axis_index("sp")
    tp = lax.axis_index("tp")
    core = lax.rem(me, 2)
    y = lax.rem(me // 2, wide)
    z = me // (2 * wide)
    rows = tok_hbm.shape[0]
    block = rows * parts
    heads = gate_hbm.shape[0]
    pc = wk_hbm.shape[1]
    local_kv = pc // HEAD_DIM
    group = heads // local_kv
    qc = heads * HEAD_DIM
    kw = pc if pc % LANES == 0 else 2 * pc
    joined = pc % LANES == 0
    pieces = chunk_count(parts)
    part = rows // pieces
    items = 2 + (parts - 1) * pieces

    def index(zz, yy, cc):
        return (zz * wide + yy) * 2 + cc

    half = n // 2
    mine = z * wide + y

    def slot(zz, yy, cc):
        return cc * half + zz * wide + yy

    own = slot(z, y, core)

    def peer(j):
        return lax.rem(tp + j, parts)

    loads = [
        pltpu.make_async_copy(src, dst, load_sem.at[i])
        for i, (src, dst) in enumerate(
            (
                (tok_hbm, tok.at[0]),
                (gate_hbm, gate_t),
                (wk_hbm, wkv.at[:, pl.ds(0, pc)] if joined else wkv.at[0]),
                (wv_hbm, wkv.at[:, pl.ds(pc, pc)] if joined else wkv.at[1]),
                (wq_hbm, wq),
                (wo_hbm, wo),
            )
        )
    ]
    for load in loads:
        load.start()

    kv[...] = jnp.zeros_like(kv)

    barrier = pltpu.get_barrier_semaphore()
    for j in range(1, parts):
        pl.semaphore_signal(barrier, inc=1, device_id={"tp": peer(j)})
    for j in range(1, deep):
        pl.semaphore_signal(barrier, inc=1, device_id={"sp": index(lax.rem(z + j, deep), y, core)})
    for j in range(1, wide):
        pl.semaphore_signal(barrier, inc=1, device_id={"sp": index(z, lax.rem(y + j, wide), core)})
    pl.semaphore_signal(barrier, inc=1, device_id={"sp": index(z, y, 1 - core)})
    loads[0].wait()
    loads[1].wait()

    gate[...] = gate_t[...].T
    turned = jnp.concatenate(
        [gate[pl.ds(pl.multiple_of(peer(j) * rows, rows), rows), :] for j in range(parts)], axis=0
    )
    hi, mid, low = split3(turned)
    fill = GATE_LANES - 3 * heads
    per_token = jnp.concatenate((hi, mid, low, jnp.ones((block, fill), F32)), axis=1)
    pack = LANES // GATE_LANES
    span = block // pack
    gates[own] = jnp.concatenate(
        [per_token[j * span : (j + 1) * span, :] for j in range(pack)], axis=1
    ).astype(BF)

    pl.semaphore_wait(barrier, parts - 1 + deep - 1 + wide - 1 + 1)

    tok_copies = {}
    for j in range(1, parts):
        for q in range(pieces):
            at = pl.ds(q * part, part)
            copy = pltpu.make_async_remote_copy(
                src_ref=tok.at[0, at],
                dst_ref=tok.at[parts - j, at],
                send_sem=tok_send.at[j, q],
                recv_sem=tok_recv.at[parts - j, q],
                device_id={"tp": peer(j)},
            )
            copy.start()
            tok_copies[j, q] = copy

    def view(item, who):
        if item == 0:
            return gates.at[who]
        if item == 1:
            return kv.at[who, pl.ds(0, rows)]
        return kv.at[who, pl.ds(rows + (item - 2) * part, part)]

    def push(item, who, send_sem, target):
        return pltpu.make_async_remote_copy(
            src_ref=view(item, who),
            dst_ref=view(item, who),
            send_sem=send_sem,
            recv_sem=recv.at[item, who],
            device_id={"sp": target},
        )

    def arrived(item, who):
        push(item, who, z_send.at[item, 0], me).wait_recv()

    def z_push(item, zz):
        return push(item, own, z_send.at[item, zz], index(zz, y, core))

    def y_push(item, zz, yy):
        return push(item, slot(zz, y, core), y_send.at[item, zz, yy], index(z, yy, core))

    def c_push(item, zz, yy):
        return push(item, slot(zz, yy, core), c_send.at[item, zz, yy], index(z, y, 1 - core))

    def loop(lo, hi, body):
        def step(i, carry):
            body(i)
            return carry

        lax.fori_loop(lo, hi, step, 0)

    def stage_own(item):
        loop(z + 1, deep, lambda zz: z_push(item, deep + z - zz).start())
        loop(y + 1, wide, lambda yy: y_push(item, z, yy).start())

        @pl.when(core == 0)
        def _():
            c_push(item, z, y).start()

    def other_y(fn):
        loop(0, y, fn)
        loop(y + 1, wide, fn)

    def stage_z(item):
        def one(zz):
            arrived(item, slot(zz, y, core))
            other_y(lambda yy: y_push(item, zz, yy).start())
            c_push(item, zz, y).start()

        loop(0, z, one)

    def stage_y(item):
        def at(zz, yy):
            arrived(item, slot(zz, yy, core))
            c_push(item, zz, yy).start()

        loop(0, z, lambda zz: other_y(lambda yy: at(zz, yy)))
        loop(0, y, lambda yy: at(z, yy))

    def stage_c(item):
        def at(zz, yy):
            arrived(item, slot(zz, yy, 1 - core))

        loop(0, z, lambda zz: loop(0, wide, lambda yy: at(zz, yy)))
        loop(0, y, lambda yy: at(z, yy))

        @pl.when(core == 1)
        def _():
            at(z, y)

    def drain(item):
        loop(z + 1, deep, lambda zz: z_push(item, zz).wait_send())
        loop(y + 1, wide, lambda yy: y_push(item, z, yy).wait_send())

        @pl.when(core == 0)
        def _():
            c_push(item, z, y).wait_send()

        def one(zz):
            other_y(lambda yy: y_push(item, zz, yy).wait_send())
            loop(0, wide, lambda yy: c_push(item, zz, yy).wait_send())

        loop(0, z, one)
        loop(0, y, lambda yy: c_push(item, z, yy).wait_send())

    stage_own(0)

    def project_kv(j, lo, size):
        x = tok[j, lo : lo + size, :]
        if joined:
            both = jnp.dot(x, wkv[...], preferred_element_type=F32)
        else:
            both = jnp.concatenate(
                [jnp.dot(x, wkv[i], preferred_element_type=F32) for i in range(2)], axis=1
            )
        kv[own, j * rows + lo : j * rows + lo + size, :] = both.astype(BF)

    def project_q(j):
        qrows[j * rows : (j + 1) * rows, :] = jnp.dot(
            tok[j], wq[...], preferred_element_type=F32
        ).astype(BF)

    loads[2].wait()
    loads[3].wait()
    project_kv(0, 0, rows)
    stage_own(1)
    loads[4].wait()
    project_q(0)
    stage_z(0)
    stage_z(1)
    stage_y(0)
    stage_y(1)
    for item in range(2, items):
        j, q = 1 + (item - 2) // pieces, (item - 2) % pieces
        tok_copies[parts - j, q].wait_recv()
        project_kv(j, q * part, part)
        stage_own(item)
    for j in range(1, parts):
        project_q(j)

    scale = HEAD_DIM ** (-0.5)
    lane = lax.broadcasted_iota(jnp.int32, (block, LANES), 1)
    query = qrows[...].astype(F32) * scale
    for h in range(heads):
        g = h // group
        place = []
        if g > 0:
            place.append(jnp.zeros((block, g * HEAD_DIM), F32))
        place.append(query[:, h * HEAD_DIM : (h + 1) * HEAD_DIM])
        if kw - (g + 1) * HEAD_DIM > 0:
            place.append(jnp.zeros((block, kw - (g + 1) * HEAD_DIM), F32))
        at_gate = (lane == h) | (lane == heads + h) | (lane == 2 * heads + h)
        side = jnp.where(at_gate, -1.0, 0.0)
        for i, piece in enumerate((hi, mid, low)):
            side = jnp.where(lane == 3 * heads + i, piece[:, h : h + 1], side)
        both = jnp.concatenate(place + [side], axis=1)
        qg[:, h * block : (h + 1) * block] = both.T.astype(BF)

    def unpack_gates(who):
        packed = gates[who].astype(F32)
        out = [packed] + [
            pltpu.roll(packed, LANES - j * GATE_LANES, 1) for j in range(1, pack)
        ]
        sides[who] = jnp.concatenate(out, axis=0).astype(BF)

    sides[...] = jnp.zeros_like(sides)
    loop(core * half, core * half + mine + 1, unpack_gates)
    big = math.gcd(8, half)
    steps = mine // big
    every = tuple(range(local_kv))

    def attend(cc, step, lo, size, last):
        first = cc * half + step * big
        width = big * size
        keyval = kv[pl.ds(first, big), lo : lo + size, :].reshape(width, 2 * pc)
        gate_part = sides[pl.ds(first, big), lo : lo + size, :].reshape(width, LANES)
        left = jnp.concatenate((keyval[:, :kw], gate_part), axis=1)
        value_t = keyval[:, pc:].astype(F32).T.astype(BF)
        if last:
            row = lax.broadcasted_iota(jnp.int32, (width, block), 0)
            which = 2 * (step * big + row // size) + cc
            key_at = lax.rem(lo + lax.rem(row, size) + tp * rows, block)
            query_at = lax.rem(lax.broadcasted_iota(jnp.int32, (width, block), 1) + tp * rows, block)
            key_pos, query_pos = which * block + key_at, me * block + query_at
            bias = jnp.where(key_pos <= query_pos, 0.0, NEG_FILL)
            bias = jnp.concatenate([bias] * group, axis=1)
        for g in every:
            at = slice(g * group * block, (g + 1) * group * block)
            scores = jnp.dot(left, qg[:, at], preferred_element_type=F32)
            if last:
                scores = scores + bias
            old_max = run_max[:, at]
            new_max = jnp.maximum(old_max, jnp.max(scores, axis=0, keepdims=True))
            weights = jnp.exp(scores - new_max)
            total = jnp.sum(weights, axis=0, keepdims=True)
            gained = jnp.dot(
                value_t[g * HEAD_DIM : (g + 1) * HEAD_DIM, :],
                weights.astype(BF),
                preferred_element_type=F32,
            )
            factor = jnp.exp(old_max - new_max)
            run_sum[:, at] = run_sum[:, at] * factor + total
            acc[:, at] = acc[:, at] * factor + gained
            run_max[:, at] = new_max

    run_max[...] = jnp.full_like(run_max, NEG_FILL)
    run_sum[...] = jnp.zeros_like(run_sum)
    acc[...] = jnp.zeros_like(acc)
    def attend_all(cc, lo, size):
        loop(0, steps, lambda i: attend(cc, i, lo, size, False))
        attend(cc, steps, lo, size, True)

    for item in range(2, items):
        stage_z(item)
    attend_all(core, 0, rows)
    stage_c(0)
    stage_c(1)
    loop((1 - core) * half, (1 - core) * half + mine + core, unpack_gates)
    attend_all(1 - core, 0, rows)
    for item in range(2, items):
        stage_y(item)
    attend_all(core, rows, block - rows)
    for item in range(2, items):
        stage_c(item)
    attend_all(1 - core, rows, block - rows)

    att_copies = []
    gc = qc // local_kv
    for g in every:
        at = slice(g * group * block, (g + 1) * group * block)
        done = acc[:, at] / run_sum[:, at]
        stacked = jnp.concatenate(
            [done[:, h * block : (h + 1) * block] for h in range(group)], axis=0
        )
        att[g] = stacked.T.astype(BF).reshape(parts, rows, gc)
        for j in range(1, parts):
            copy = pltpu.make_async_remote_copy(
                src_ref=att.at[g, j],
                dst_ref=att_in.at[g, parts - j],
                send_sem=att_send.at[g, j],
                recv_sem=att_recv.at[g, parts - j],
                device_id={"tp": peer(j)},
            )
            copy.start()
            att_copies.append(copy)
    loads[5].wait()

    def w_rows(g, j):
        return wo[pl.ds(pl.multiple_of(peer(j) * qc + g * gc, gc), gc), :]

    mixed = None
    for g in every:
        term = jnp.dot(att[g, 0], w_rows(g, 0), preferred_element_type=F32)
        mixed = term if mixed is None else mixed + term
    for g in every:
        for j in range(1, parts):
            att_copies[g * (parts - 1) + parts - j - 1].wait_recv()
            mixed = mixed + jnp.dot(att_in[g, j], w_rows(g, j), preferred_element_type=F32)
    out_ref[...] = mixed.astype(BF)

    for copy in list(tok_copies.values()) + att_copies:
        copy.wait_send()
    for item in range(items):
        drain(item)


def shards(n, parts, tokens, w_query, w_key, w_value, cum_gate, w_out):
    deep, wide = dims(n)
    rows, width = tokens.shape
    block = rows * parts
    heads = cum_gate.shape[1]
    pc = w_key.shape[1]
    qc = w_query.shape[1]
    kw = pc if pc % LANES == 0 else 2 * pc
    cols = heads * block
    span = block * GATE_LANES // LANES
    local_kv = pc // HEAD_DIM
    pieces = chunk_count(parts)
    items = 2 + (parts - 1) * pieces
    dma = pltpu.SemaphoreType.DMA
    return pl.pallas_call(
        functools.partial(kernel, n, parts),
        out_shape=jax.ShapeDtypeStruct((rows, w_out.shape[1]), BF),
        in_specs=[pl.BlockSpec(memory_space=pltpu.HBM)] * 6,
        out_specs=pl.BlockSpec(memory_space=pltpu.VMEM),
        scratch_shapes=[
            pltpu.VMEM((parts, rows, width), BF),
            pltpu.VMEM(w_query.shape, BF),
            pltpu.VMEM((width, 2 * pc) if pc % LANES == 0 else (2, width, pc), BF),
            pltpu.VMEM(w_out.shape, BF),
            pltpu.VMEM((heads, block), F32),
            pltpu.VMEM((block, heads), F32),
            pltpu.VMEM((block, qc), BF),
            pltpu.VMEM((n, block, 2 * pc), BF),
            pltpu.VMEM((n, span, LANES), BF),
            pltpu.VMEM((n, block, LANES), BF),
            pltpu.VMEM((kw + LANES, cols), BF),
            pltpu.VMEM((1, cols), F32),
            pltpu.VMEM((1, cols), F32),
            pltpu.VMEM((HEAD_DIM, cols), F32),
            pltpu.VMEM((local_kv, parts, rows, qc // local_kv), BF),
            pltpu.VMEM((local_kv, parts, rows, qc // local_kv), BF),
            dma((6,)),
            dma((parts, pieces)),
            dma((parts, pieces)),
            dma((local_kv, parts)),
            dma((local_kv, parts)),
            dma((items, deep)),
            dma((items, deep, wide)),
            dma((items, deep, wide)),
            dma((items, n)),
        ],
        compiler_params=pltpu.CompilerParams(
            collective_id=0, has_side_effects=True, vmem_limit_bytes=VMEM_LIMIT
        ),
    )(tokens, w_query, w_key, w_value, cum_gate.T, w_out)


def solution(mesh):
    n, parts = mesh.shape["sp"], mesh.shape["tp"]
    placed = (
        P(("sp", "tp"), None),
        P(None, "tp"),
        P(None, "tp"),
        P(None, "tp"),
        P("sp", "tp"),
        P(),
    )
    return jax.shard_map(
        functools.partial(shards, n, parts),
        mesh=mesh,
        in_specs=placed,
        out_specs=P(("sp", "tp"), None),
        check_vma=False,
    )
```
